32 devices in a mesh: ep: 8 (over z, x), tp: 4 (over y, core).
Axes of the slice: x: 2, y: 2, z: 4, core: 2. Of those that a mesh axis runs over, the one named last changes fastest.
Arguments:
- tokens: bfloat16 [2048, 2048], P('ep', 'tp'), may hold values from -6 to 6
- row_ids: int32 [2048, 16], P('ep'), may hold values from 0 to 32767, as said below
- row_gates: float32 [2048, 16], P('ep'), may hold values from 0.02 to 0.5
- key_table: bfloat16 [32768, 2048], P('ep', 'tp'), may hold values from -0.125 to 0.125
- value_table: bfloat16 [32768, 2048], P('ep', 'tp'), may hold values from -14 to 14
- norm_gain: float32 [2048], P('tp'), may hold values from 0.1 to 1.9
Outputs:
- output: bfloat16 [2048, 2048], P('ep', 'tp')
The draws below stay inside these ranges and needn't reach their ends.
Inputs may be any that keep to these rules, and one draw needn't show every extreme that they name: `row_ids`: table row r belongs to index r // 4096 of ep. The 256 tokens of one index of ep choose at most 1536 rows belonging to any one index, exactly 1536 from some index, and at least one from every index.
All inputs are finite; a program needn't handle non-finite values.
Results may differ from the reference program's by a relative error of at most 0.0065.
Values may be sent and summed in bfloat16 or wider, within the bound.
A program may use at most 64 MiB of HBM per device.

```python
import math
import jax
import jax.numpy as jnp
from jax import lax

D = 2048
PICKS = 16
EXP_DEV = 4096
TOK_DEV = 256
EXPERTS = 32768
TOKENS = 2048
CAP = 1536


def draw_row_ids(key, part):
    devices = TOKENS // TOK_DEV
    per_device = TOK_DEV * PICKS
    key_hot, key_order, key_local = jax.random.split(key, 3)
    hottest = jax.random.randint(key_hot, (devices, 1), 0, devices)
    slot = jnp.arange(per_device, dtype=jnp.int32)[None, :]
    spread = (slot - CAP) % (devices - 1)
    others = spread + (spread >= hottest).astype(jnp.int32)
    owner = jnp.where(slot < CAP, hottest, others)
    local = jax.random.randint(key_local, (devices, per_device), 0, EXP_DEV)
    order = jax.vmap(lambda k: jax.random.permutation(k, per_device))(jax.random.split(key_order, devices))
    chosen = jnp.take_along_axis(owner * EXP_DEV + local, order.astype(jnp.int32), axis=1)
    return chosen.reshape(TOKENS, PICKS).astype(jnp.int32)


def draw_value_table(key, part):
    key_base, key_rough = jax.random.split(key)
    column = jnp.arange(D, dtype=jnp.float32) / D
    rough = jax.random.uniform(key_rough, (D,), jnp.float32, 0.5, 1.5)
    base = jnp.clip(jax.random.normal(key_base, (EXPERTS, D), jnp.float32), -4.5, 4.5)
    rising = jnp.exp(math.log(4.0) * column)
    return (base * rising * rough * PICKS ** (-0.5)).astype(jnp.bfloat16)


def levels(stream_key, shape, pieces, least, high):
    level = 1.0
    for axis_at, blocks in pieces:
        steps = jax.random.uniform(jax.random.fold_in(jax.random.fold_in(stream_key, 6), axis_at), (blocks,), jnp.float32, least / len(pieces), high / len(pieces))
        level = level * jnp.repeat(jnp.exp(steps), shape[axis_at] // blocks).reshape((-1,) + (1,) * (len(shape) - 1 - axis_at))
    return level


def noise(key, dims, width, reach, pieces=(), held_as=jnp.bfloat16):
    array = width * jax.random.normal(key, dims, jnp.float32)
    if pieces:
        array = array * levels(key, dims, pieces, -0.22, 0.18)
    return jnp.clip(array, -reach, reach).astype(held_as)


def setup_inputs(seed: int = 0) -> dict:
    streams_of = jax.random.split(jax.random.key(seed), 7)
    return {
        "tokens": noise(streams_of[0], (TOKENS, D), 1.0, 6.0, ((0, 8), (1, 4))),
        "row_ids": draw_row_ids(jax.random.fold_in(streams_of[6], 71), 0),
        "row_gates": jnp.clip(jnp.exp(math.log(0.5) - 3.218876 * jax.random.uniform(streams_of[2], (TOKENS, PICKS), jnp.float32) ** levels(streams_of[2], (TOKENS, PICKS), ((0, 8),), -0.2, 0.2)), 0.02, 0.5),
        "key_table": noise(streams_of[3], (EXPERTS, D), D ** -0.5, 0.125, ((0, 8), (1, 4))),
        "value_table": draw_value_table(jax.random.fold_in(streams_of[6], 71), 0),
        "norm_gain": jnp.clip(1.0 + 0.18 * jax.random.normal(streams_of[5], (D,), jnp.float32), 0.1, 1.9),
    }


def reference(tokens, row_ids, row_gates, key_table, value_table, norm_gain):
    blocks = TOKENS // TOK_DEV

    def one_block(args):
        vectors, chosen, weights = args
        keys = key_table[chosen].astype(jnp.float32)
        score = jnp.einsum('td,tkd->tk', vectors.astype(jnp.float32), keys)
        hidden = jax.nn.gelu(score, approximate=False) * weights
        values = value_table[chosen].astype(jnp.float32)
        return jnp.einsum('tk,tkd->td', hidden, values)
    mixed = lax.map(one_block, (tokens.reshape(blocks, TOK_DEV, D), row_ids.reshape(blocks, TOK_DEV, PICKS), row_gates.reshape(blocks, TOK_DEV, PICKS)))
    mixed = mixed.reshape(TOKENS, D)
    strength = lax.optimization_barrier(jnp.mean(mixed * mixed, axis=-1, keepdims=True))
    return (mixed * lax.rsqrt(strength + 1e-06) * norm_gain).astype(jnp.bfloat16)
```

```python
import functools

import jax
import jax.numpy as jnp
from jax import lax
from jax.experimental import pallas as pl
from jax.experimental.pallas import tpu as pltpu
from jax.sharding import PartitionSpec as P

ROW = 256
LANES = 128
MESH = pl.DeviceIdType.MESH


def cycle_of(n):
    x = 1
    while 4 * x * x <= n:
        x *= 2
    z = n // x
    if x == 1 or z % 2:
        return list(range(n))
    out = []
    for row in range(z):
        cols = range(1, x) if row % 2 == 0 else range(x - 1, 0, -1)
        out += [row * x + col for col in cols]
    return out + [row * x for row in range(z - 1, -1, -1)]


def look(table, i):
    n = len(table)
    total = 0
    for k, v in enumerate(table):
        total = total + v * ((n * n - (i - k) * (i - k)) // (n * n))
    return total


def greet(n, tps, me, order):
    pos = look([order.index(i) for i in range(n)], me)
    right = look(order, lax.rem(pos + 1, n))
    left = look(order, lax.rem(pos + n - 1, n))
    mine = lax.axis_index("tp")
    barrier = pltpu.get_barrier_semaphore()
    for peer in (left, right):
        pl.semaphore_signal(barrier, inc=1, device_id=(peer, mine), device_id_type=MESH)
    for k in range(1, tps):
        pl.semaphore_signal(
            barrier, inc=1, device_id=(me, lax.rem(mine + k, tps)), device_id_type=MESH
        )
    pl.semaphore_wait(barrier, 2 + tps - 1)
    return pos, right, left, mine


def remote(src, dst, send, recv, device):
    return pltpu.make_async_remote_copy(
        src_ref=src, dst_ref=dst, send_sem=send, recv_sem=recv, device_id=device, device_id_type=MESH
    )


def kernel(n, tps, picks, order, *refs):
    x_ref, meta_ref, key_hbm, value_hbm, gain_ref, out_ref = refs[:6]
    key_ref, value_ref, xall, metas, s_ref, part, got_ref, w_ref = refs[6:14]
    own, mix_ref, sent, came, sq_ref, sq_got = refs[14:20]
    xs, xr, ms, mr, ps, pr, ss, sr, qs, qr, kv = refs[20:]
    block, width = x_ref.shape
    half = block // 2
    experts = key_ref.shape[0]
    lines = meta_ref.shape[1] // 2
    cuts = xs.shape[2]
    rows = half // cuts
    key_copy = pltpu.make_async_copy(key_hbm, key_ref, kv.at[0])
    value_copy = pltpu.make_async_copy(value_hbm, value_ref, kv.at[1])
    key_copy.start()
    me = lax.axis_index("ep")
    pos, right, left, mine = greet(n, tps, me, order)
    base = me * experts
    peers = (right, left)

    def x_copy(d, step, c, first=False):
        at = pl.ds(d * half + c * rows, rows)
        src = x_ref.at[at] if first else xall.at[step, at]
        return remote(
            src, xall.at[step + 1, at], xs.at[d, step, c], xr.at[d, step, c], (peers[d], mine)
        )

    def m_copy(d, step, first=False):
        src = meta_ref.at[d] if first else metas.at[step, d]
        return remote(src, metas.at[step + 1, d], ms.at[d, step], mr.at[d, step], (peers[d], mine))

    def p_copy(s, k):
        return remote(
            part.at[s],
            got_ref.at[s, k - 1],
            ps.at[s, k - 1],
            pr.at[s, k - 1],
            (me, lax.rem(mine + k, tps)),
        )

    def r_copy(d, s, c):
        return remote(
            sent.at[s, d, c], came.at[s, d, c], ss.at[d, s, c], sr.at[d, s, c], (peers[d], mine)
        )

    for c in range(cuts):
        for d in (0, 1):
            x_copy(d, 0, c, True).start()
            if c == 0:
                m_copy(d, 0, True).start()
    xall[0] = x_ref[...]
    metas[0] = meta_ref[...]
    value_copy.start()
    key_copy.wait()

    per_half = LANES // picks
    sub = lax.broadcasted_iota(jnp.int32, (per_half, LANES), 0)
    lane = lax.broadcasted_iota(jnp.int32, (per_half, LANES), 1)
    own_lane = sub == lane // picks
    per = ROW // picks
    tall = experts // ROW * per
    lane_token = lax.broadcasted_iota(jnp.int32, (1, ROW), 1) // picks
    tall_iota = lax.broadcasted_iota(jnp.int32, (tall, ROW), 0)
    lo_iota = lax.broadcasted_iota(jnp.int32, (ROW, ROW), 0)
    spans = 2 * lines
    wide = experts // spans

    def gather_on(s, c):
        @pl.when(s < n)
        def _():
            for d in (0, 1):
                x_copy(d, s - 1, c).wait_recv()

                @pl.when(s < n - 1)
                def _():
                    x_copy(d, s, c).start()

                if c == 0:
                    m_copy(d, s - 1).wait_recv()

                    @pl.when(s < n - 1)
                    def _():
                        m_copy(d, s).start()

    def score(s, i):
        at = slice(i * wide, (i + 1) * wide)
        s_ref[:, at] = lax.dot_general(
            xall[s],
            key_ref[at, :],
            (((1,), (1,)), ((), ())),
            preferred_element_type=jnp.float32,
        )

    def choose(s, i):
        d, r = i // lines, i % lines
        for h2 in range(ROW // LANES):
            lanes = slice(h2 * LANES, (h2 + 1) * LANES)
            ids = metas[s, d, r : r + 1, lanes].astype(jnp.int32) - base
            ids = jnp.broadcast_to(ids, (per_half, LANES))
            owned = (ids >= 0) & (ids < experts)
            hi = jnp.where(owned, ids >> 7, -1)
            lo = jnp.where(owned, ids & (LANES - 1), 0)
            row = i * per + h2 * per_half
            acc = jnp.zeros((per_half, LANES), jnp.float32)
            for h in range(experts // LANES):
                tile = s_ref[row : row + per_half, h * LANES : (h + 1) * LANES]
                acc = jnp.where(hi == h, jnp.take_along_axis(tile, lo, axis=1), acc)
            part[s, i : i + 1, lanes] = jnp.sum(
                jnp.where(own_lane, acc, 0.0), axis=0, keepdims=True
            )

    def build(s, i):
        d, r = i // lines, i % lines
        total = part[s, i : i + 1, :]
        for k in range(1, tps):
            total = total + got_ref[s, k - 1, i : i + 1, :]
        h = 0.5 * total * (1.0 + lax.erf(total * (0.5**0.5))) * metas[s, d, lines + r : lines + r + 1, :]
        ids = metas[s, d, r : r + 1, :].astype(jnp.int32) - base
        owned = (ids >= 0) & (ids < experts)
        code = jnp.where(owned, (ids >> 8) * per + lane_token, -1)
        lo = ids & (ROW - 1)
        a = jnp.where(tall_iota == code, h, 0.0).astype(jnp.bfloat16)
        b = jnp.where(lo_iota == lo, 1.0, 0.0).astype(jnp.bfloat16)
        w = lax.dot_general(
            a, b, (((1,), (1,)), ((), ())), preferred_element_type=jnp.float32
        ).astype(jnp.bfloat16)
        for c in range(experts // ROW):
            w_ref[i * per : (i + 1) * per, c * ROW : (c + 1) * ROW] = w[c * per : (c + 1) * per, :]

    def send_part(s):
        for k in range(1, tps):
            p_copy(s, k).start()

    def wait_part(s):
        for k in range(1, tps):
            p_copy(s, k).wait()

    def blend(s, choosing):
        pieces = 4
        deep = experts // pieces
        mixed = None
        for q in range(pieces):
            at = slice(q * deep, (q + 1) * deep)
            dot = jnp.dot(w_ref[:, at], value_ref[at, :], preferred_element_type=jnp.float32)
            mixed = dot if mixed is None else mixed + dot
            if choosing is not None:
                for i in range(q * spans // pieces, (q + 1) * spans // pieces):
                    choose(choosing, i)
        mix_ref[...] = mixed

    def reduce_on(s, c):
        @pl.when((s >= 1) & (s < n))
        def _():
            for d in (0, 1):
                at = slice(d * half + c * rows, d * half + (c + 1) * rows)

                @pl.when(s >= 2)
                def _():
                    r_copy(d, s - 2, c).wait_recv()
                    sent[s - 1, d, c] = (
                        mix_ref[at, :] + came[s - 2, d, c].astype(jnp.float32)
                    ).astype(jnp.bfloat16)

                @pl.when(s == 1)
                def _():
                    sent[0, d, c] = mix_ref[at, :].astype(jnp.bfloat16)

                r_copy(d, s - 1, c).start()

    def keep(s):
        @pl.when(s == 0)
        def _():
            own[...] = mix_ref[...]

    def lead(t, carry):
        for i in range(spans):
            score(t, i)
        for i in range(spans):
            choose(t, i)
        send_part(t)
        for c in range(cuts):
            gather_on(t + 1, c)
        return carry

    lax.fori_loop(0, 2, lead, 0)
    value_copy.wait()
    first = cuts // 2

    def steady(t, carry):
        wait_part(t - 2)
        for i in range(spans):
            score(t, i)
            build(t - 2, i)
        for c in range(first):
            gather_on(t + 1, c)
        for c in range(first, cuts):
            reduce_on(t - 3, c)
        blend(t - 2, t)
        send_part(t)
        keep(t - 2)
        for c in range(first, cuts):
            gather_on(t + 1, c)
        for c in range(first):
            reduce_on(t - 2, c)
        return carry

    lax.fori_loop(2, n, steady, 0)

    def last(t, carry):
        wait_part(t - 2)
        for i in range(spans):
            build(t - 2, i)
        for c in range(first, cuts):
            reduce_on(t - 3, c)
        blend(t - 2, None)
        keep(t - 2)
        for c in range(first):
            reduce_on(t - 2, c)
        return carry

    lax.fori_loop(n, n + 2, last, 0)
    for c in range(first, cuts):
        reduce_on(n - 1, c)

    ones = jnp.ones((8, width), jnp.float32)
    for c in range(cuts):
        for d in (0, 1):
            at = slice(d * half + c * rows, d * half + (c + 1) * rows)
            r_copy(d, n - 2, c).wait_recv()
            own[at, :] = own[at, :] + came[n - 2, d, c].astype(jnp.float32)
    mixed = own[...]
    square = lax.dot_general(
        ones,
        mixed * mixed,
        (((1,), (1,)), ((), ())),
        precision=lax.Precision.HIGHEST,
        preferred_element_type=jnp.float32,
    )
    sq_ref[...] = square

    def q_copy(k):
        return remote(
            sq_ref, sq_got.at[k - 1], qs.at[k - 1], qr.at[k - 1], (me, lax.rem(mine + k, tps))
        )

    for k in range(1, tps):
        q_copy(k).start()

    def drain(s, carry):
        for d in (0, 1):
            m_copy(d, s).wait_send()
            for c in range(cuts):
                x_copy(d, s, c).wait_send()
                r_copy(d, s, c).wait_send()
        return carry

    lax.fori_loop(0, n - 1, drain, 0)
    for k in range(1, tps):
        q_copy(k).wait()
    total = square
    for k in range(1, tps):
        total = total + sq_got[k - 1]
    scale = lax.rsqrt(total / (width * tps) + 1e-06)
    column = lax.dot_general(
        scale,
        jnp.full((8, LANES), 0.125, jnp.float32),
        (((0,), (0,)), ((), ())),
        precision=lax.Precision.HIGHEST,
        preferred_element_type=jnp.float32,
    )
    for c in range(width // LANES):
        at = slice(c * LANES, (c + 1) * LANES)
        out_ref[:, at] = (own[:, at] * column * gain_ref[:, at]).astype(jnp.bfloat16)


def body(tokens, row_ids, row_gates, key_table, value_table, norm_gain):
    block, width = tokens.shape
    picks = row_ids.shape[1]
    experts = key_table.shape[0]
    n, tps = lax.axis_size("ep"), lax.axis_size("tp")
    half = block // 2
    lines = half * picks // ROW
    cuts = 2
    rows = half // cuts
    meta = jnp.concatenate(
        [
            row_ids.astype(jnp.float32).reshape(2, lines, ROW),
            row_gates.reshape(2, lines, ROW),
        ],
        axis=1,
    )
    whole = pl.BlockSpec(memory_space=pltpu.VMEM)
    hbm = pl.BlockSpec(memory_space=pl.ANY)
    dma = pltpu.SemaphoreType.DMA
    bf16, f32 = jnp.bfloat16, jnp.float32
    return pl.pallas_call(
        functools.partial(kernel, n, tps, picks, cycle_of(n)),
        out_shape=jax.ShapeDtypeStruct((block, width), bf16),
        in_specs=[whole, whole, hbm, hbm, whole],
        out_specs=whole,
        scratch_shapes=[
            pltpu.VMEM((experts, width), bf16),
            pltpu.VMEM((experts, width), bf16),
            pltpu.VMEM((n, block, width), bf16),
            pltpu.VMEM((n, 2, 2 * lines, ROW), f32),
            pltpu.VMEM((block, experts), f32),
            pltpu.VMEM((n, 2 * lines, ROW), f32),
            pltpu.VMEM((n, tps - 1, 2 * lines, ROW), f32),
            pltpu.VMEM((block, experts), bf16),
            pltpu.VMEM((block, width), f32),
            pltpu.VMEM((block, width), f32),
            pltpu.VMEM((n - 1, 2, cuts, rows, width), bf16),
            pltpu.VMEM((n - 1, 2, cuts, rows, width), bf16),
            pltpu.VMEM((8, block), f32),
            pltpu.VMEM((tps - 1, 8, block), f32),
            dma((2, n - 1, cuts)),
            dma((2, n - 1, cuts)),
            dma((2, n - 1)),
            dma((2, n - 1)),
            dma((n, tps - 1)),
            dma((n, tps - 1)),
            dma((2, n - 1, cuts)),
            dma((2, n - 1, cuts)),
            dma((tps - 1,)),
            dma((tps - 1,)),
            dma((2,)),
        ],
        compiler_params=pltpu.CompilerParams(collective_id=0, has_side_effects=True),
    )(tokens, meta, key_table, value_table, norm_gain.reshape(1, -1))


def solution(mesh):
    in_specs = (P("ep", "tp"), P("ep", None), P("ep", None), P("ep", "tp"), P("ep", "tp"), P("tp"))
    out_specs = P("ep", "tp")
    return jax.shard_map(body, mesh=mesh, in_specs=in_specs, out_specs=out_specs, check_vma=False)
```

```python
import functools

import jax
import jax.numpy as jnp
from jax import lax
from jax.experimental import pallas as pl
from jax.experimental.pallas import tpu as pltpu
from jax.sharding import PartitionSpec as P

ROW = 256
LANES = 128
MESH = pl.DeviceIdType.MESH


def cycle_of(n):
    x = 1
    while 4 * x * x <= n:
        x *= 2
    z = n // x
    if x == 1 or z % 2:
        return list(range(n))
    out = []
    for row in range(z):
        cols = range(1, x) if row % 2 == 0 else range(x - 1, 0, -1)
        out += [row * x + col for col in cols]
    return out + [row * x for row in range(z - 1, -1, -1)]


def look(table, i):
    n = len(table)
    total = 0
    for k, v in enumerate(table):
        total = total + v * ((n * n - (i - k) * (i - k)) // (n * n))
    return total


def hello(n, tps, me, order):
    pos = look([order.index(i) for i in range(n)], me)
    right = look(order, lax.rem(pos + 1, n))
    left = look(order, lax.rem(pos + n - 1, n))
    mine = lax.axis_index("tp")
    barrier = pltpu.get_barrier_semaphore()
    for peer in (left, right):
        pl.semaphore_signal(barrier, inc=1, device_id=(peer, mine), device_id_type=MESH)
    for k in range(1, tps):
        pl.semaphore_signal(
            barrier, inc=1, device_id=(me, lax.rem(mine + k, tps)), device_id_type=MESH
        )
    return right, left, mine


def greeted(tps):
    pl.semaphore_wait(pltpu.get_barrier_semaphore(), 2 + tps - 1)


def remote(src, dst, send, recv, device):
    return pltpu.make_async_remote_copy(
        src_ref=src, dst_ref=dst, send_sem=send, recv_sem=recv, device_id=device, device_id_type=MESH
    )


def kernel(n, tps, picks, order, *refs):
    x_hbm, ids_hbm, gates_hbm, key_hbm, value_hbm, gain_hbm, out_ref = refs[:7]
    key_ref, value_ref, xall, metas, s_ref, part, got_ref, w_ref = refs[7:15]
    mix_ref, sent, came, sq_ref, sq_got = refs[15:20]
    ids_ref, gates_ref, gain_ref = refs[20:23]
    xr, mr, pr, sr, qr, ends, kv = refs[23:]
    cuts, rows, width = xall.shape[1], xall.shape[3], xall.shape[4]
    pair = 2 * rows
    block = cuts * pair
    half = block // 2
    experts = key_ref.shape[0]
    lines = metas.shape[2] // 2
    me = lax.axis_index("ep")
    right, left, mine = hello(n, tps, me, order)
    ids_copy = pltpu.make_async_copy(ids_hbm, ids_ref, kv.at[0])
    gates_copy = pltpu.make_async_copy(gates_hbm, gates_ref, kv.at[1])
    key_copy = pltpu.make_async_copy(key_hbm, key_ref, kv.at[3])
    value_copy = pltpu.make_async_copy(value_hbm, value_ref, kv.at[4])
    gain_copy = pltpu.make_async_copy(gain_hbm, gain_ref, kv.at[5])
    ids_copy.start()
    gates_copy.start()
    for c in range(cuts):
        for d in (0, 1):
            pltpu.make_async_copy(
                x_hbm.at[pl.ds(d * half + c * rows, rows)], xall.at[0, c, d], kv.at[2]
            ).start()
    for copy in (key_copy, value_copy, gain_copy):
        copy.start()
    base = me * experts
    peers = (right, left)
    near = n // 2 + n // 8
    far = n - 1 - near

    def x_copy(d, step, c):
        return remote(
            xall.at[step, c, d],
            xall.at[step + 1, c, d],
            ends.at[0],
            xr.at[step, c],
            (peers[d], mine),
        )

    def m_copy(d, step):
        return remote(
            metas.at[step, d], metas.at[step + 1, d], ends.at[1], mr.at[step], (peers[d], mine)
        )

    def far_copy(d, hop, c):
        return remote(
            xall.at[lax.rem(n - hop, n), c, 1 - d],
            xall.at[n - 1 - hop, c, 1 - d],
            ends.at[0],
            xr.at[near + hop, c],
            (peers[d], mine),
        )

    def far_meta(d, hop):
        return remote(
            metas.at[lax.rem(n - hop, n), 1 - d],
            metas.at[n - 1 - hop, 1 - d],
            ends.at[1],
            mr.at[near + hop],
            (peers[d], mine),
        )

    def p_copy(s, k):
        return remote(
            part.at[s],
            got_ref.at[s, k - 1],
            ends.at[2],
            pr.at[s],
            (me, lax.rem(mine + k, tps)),
        )

    def r_copy(d, s, c):
        return remote(
            sent.at[s, c, d], came.at[s, c, d], ends.at[3], sr.at[s, c], (peers[d], mine)
        )

    def arrived(ref, sem):
        pltpu.make_async_copy(ref, ref, sem).wait()

    per_half = LANES // picks
    per = ROW // picks
    pick_row = lax.broadcasted_iota(jnp.int32, (picks, LANES), 0)
    pick_lane = lax.broadcasted_iota(jnp.int32, (picks, LANES), 1) // per_half
    ids_copy.wait()
    gates_copy.wait()
    for which, table in enumerate((ids_ref[...].astype(jnp.float32), gates_ref[...])):
        for tile in range(block // LANES):
            slanted = pltpu.roll(
                table[:, tile * LANES : (tile + 1) * LANES], 0, 1, stride=per_half, stride_axis=0
            )
            for g in range(picks):
                moved = pltpu.roll(slanted, (LANES - g * per_half) % LANES, 1) if g else slanted
                line = jnp.sum(
                    jnp.where(pick_row == pick_lane, moved, 0.0), axis=0, keepdims=True
                )
                i, h2 = divmod(tile * picks + g, 2)
                d, r = divmod(i, lines)
                metas[
                    0, d, which * lines + r : which * lines + r + 1, h2 * LANES : (h2 + 1) * LANES
                ] = line
    arrived(xall.at[0], kv.at[2])
    greeted(tps)
    for c in range(cuts):
        for d in (0, 1):
            x_copy(d, 0, c).start()
            if c == 0:
                m_copy(d, 0).start()

    sub = lax.broadcasted_iota(jnp.int32, (per_half, LANES), 0)
    lane = lax.broadcasted_iota(jnp.int32, (per_half, LANES), 1)
    own_lane = sub == lane % per_half
    tall = experts // ROW * per
    flat = lax.broadcasted_iota(jnp.int32, (1, ROW), 1)
    lane_token = flat // LANES * per_half + flat % per_half
    tall_iota = lax.broadcasted_iota(jnp.int32, (tall, ROW), 0)
    lo_iota = lax.broadcasted_iota(jnp.int32, (ROW, ROW), 0)
    spans = 2 * lines
    wide = experts // spans
    each = rows // per

    def place(i):
        return i // each % 2, i // (2 * each) * each + i % each

    def gather_on(s, c):
        @pl.when(s <= near)
        def _():
            arrived(xall.at[s, c], xr.at[s - 1, c])

            @pl.when(s < near)
            def _():
                for d in (0, 1):
                    x_copy(d, s, c).start()

            if c == 0:
                arrived(metas.at[s], mr.at[s - 1])

                @pl.when(s < near)
                def _():
                    for d in (0, 1):
                        m_copy(d, s).start()

    items = (far + 1) * cuts if far else 0

    def far_on(f):
        hop, c = f // cuts, f % cuts

        @pl.when(f < items)
        def _():
            @pl.when(hop > 0)
            def _():
                arrived(xall.at[n - hop, c], xr.at[near + hop - 1, c])

            @pl.when(hop < far)
            def _():
                for d in (0, 1):
                    far_copy(d, hop, c).start()

            @pl.when(c == 0)
            def _():
                @pl.when(hop > 0)
                def _():
                    arrived(metas.at[n - hop], mr.at[near + hop - 1])

                @pl.when(hop < far)
                def _():
                    for d in (0, 1):
                        far_meta(d, hop).start()

    def far_step(t, c):
        done = 2 * near - 2
        rest = -(-(items - done) // cuts)
        if c % 2:

            @pl.when(t < near)
            def _():
                far_on(2 * t - 2 + c // 2)

        @pl.when(t == near)
        def _():
            for f in range(done + c * rest, done + (c + 1) * rest):
                far_on(f)

    def score(s, i):
        at = slice(i * wide, (i + 1) * wide)
        s_ref[:, at] = lax.dot_general(
            xall[s].reshape(block, width),
            key_ref[at, :],
            (((1,), (1,)), ((), ())),
            preferred_element_type=jnp.float32,
        )

    def choose(s, i):
        d, r = place(i)
        for h2 in range(ROW // LANES):
            lanes = slice(h2 * LANES, (h2 + 1) * LANES)
            ids = metas[s, d, r : r + 1, lanes].astype(jnp.int32) - base
            ids = jnp.broadcast_to(ids, (per_half, LANES))
            owned = (ids >= 0) & (ids < experts)
            hi = jnp.where(owned, ids >> 7, -1)
            lo = jnp.where(owned, ids & (LANES - 1), 0)
            row = i * per + h2 * per_half
            acc = jnp.zeros((per_half, LANES), jnp.float32)
            for h in range(experts // LANES):
                tile = s_ref[row : row + per_half, h * LANES : (h + 1) * LANES]
                acc = jnp.where(hi == h, jnp.take_along_axis(tile, lo, axis=1), acc)
            part[s, i : i + 1, lanes] = jnp.sum(
                jnp.where(own_lane, acc, 0.0), axis=0, keepdims=True
            )

    def build(s, i):
        d, r = place(i)
        total = part[s, i : i + 1, :]
        for k in range(1, tps):
            total = total + got_ref[s, k - 1, i : i + 1, :]
        gate = metas[s, d, lines + r : lines + r + 1, :]
        h = 0.5 * total * (1.0 + lax.erf(total * (0.5**0.5))) * gate
        ids = metas[s, d, r : r + 1, :].astype(jnp.int32) - base
        owned = (ids >= 0) & (ids < experts)
        code = jnp.where(owned, (ids >> 8) * per + lane_token, -1)
        lo = ids & (ROW - 1)
        a = jnp.where(tall_iota == code, h, 0.0).astype(jnp.bfloat16)
        b = jnp.where(lo_iota == lo, 1.0, 0.0).astype(jnp.bfloat16)
        w = lax.dot_general(
            a, b, (((1,), (1,)), ((), ())), preferred_element_type=jnp.float32
        ).astype(jnp.bfloat16)
        for c in range(experts // ROW):
            w_ref[i * per : (i + 1) * per, c * ROW : (c + 1) * ROW] = w[c * per : (c + 1) * per, :]

    def send_part(s):
        for k in range(1, tps):
            p_copy(s, k).start()

    def wait_part(s):
        arrived(got_ref.at[s], pr.at[s])

    def blend(s, q, choosing):
        pieces = 2
        deep = experts // (2 * pieces)
        mixed = None
        for p in range(pieces):
            at = slice((q * pieces + p) * deep, (q * pieces + p + 1) * deep)
            dot = jnp.dot(w_ref[:, at], value_ref[at, :], preferred_element_type=jnp.float32)
            mixed = dot if mixed is None else mixed + dot
            if choosing is not None:
                count = spans // (2 * pieces)
                for i in range((q * pieces + p) * count, (q * pieces + p + 1) * count):
                    choose(choosing, i)
        slot = lax.rem(s, 2)
        mix_ref[slot] = mixed if q == 0 else mix_ref[slot] + mixed

    def reduce_on(s, c):
        @pl.when((s >= 1) & (s < n))
        def _():
            at = slice(c * pair, (c + 1) * pair)
            share = mix_ref.at[lax.rem(s, 2)]

            @pl.when(s >= 2)
            def _():
                arrived(came.at[s - 2, c], sr.at[s - 2, c])
                before = came[s - 2, c].reshape(pair, width).astype(jnp.float32)
                sent[s - 1, c] = (share[at, :] + before).astype(jnp.bfloat16).reshape(2, rows, width)

            @pl.when(s == 1)
            def _():
                sent[0, c] = share[at, :].astype(jnp.bfloat16).reshape(2, rows, width)

            for d in (0, 1):
                r_copy(d, s - 1, c).start()

    key_copy.wait()
    far_on(0)
    for i in range(spans):
        score(0, i)
    for i in range(spans):
        choose(0, i)
    send_part(0)
    for c in range(cuts):
        gather_on(1, c)
    far_on(1)

    def lead(t, carry):
        for i in range(spans):
            score(t, i)
        for c in range(cuts // 2):
            gather_on(t + 1, c)

            @pl.when(t > 1)
            def _():
                far_step(t, c)

        for i in range(spans):
            choose(t, i)
        send_part(t)
        for c in range(cuts // 2, cuts):
            gather_on(t + 1, c)

            @pl.when(t > 1)
            def _():
                far_step(t, c)

        return carry

    lax.fori_loop(1, 3, lead, 0)
    value_copy.wait()

    def steady(t, carry):
        wait_part(t - 2)
        for q in (0, 1):
            for i in range(q * spans // 2, (q + 1) * spans // 2):
                score(t, i)
                build(t - 2, i)
            gather_on(t + 1, q)
            far_step(t, q)
            reduce_on(t - 3, 1 + q)
        blend(t - 2, 0, t)
        gather_on(t + 1, 2)
        far_step(t, 2)
        reduce_on(t - 3, 3)
        blend(t - 2, 1, t)
        send_part(t)
        gather_on(t + 1, 3)
        far_step(t, 3)
        reduce_on(t - 2, 0)
        return carry

    lax.fori_loop(3, n, steady, 0)

    def last(t, carry):
        slot = lax.rem(t - 2, n)
        wait_part(slot)
        for q in (0, 1):
            for i in range(q * spans // 2, (q + 1) * spans // 2):
                build(slot, i)
            reduce_on(t - 3, 1 + q)
        blend(slot, 0, None)
        reduce_on(t - 3, 3)
        blend(slot, 1, None)
        reduce_on(t - 2, 0)
        return carry

    lax.fori_loop(n, n + 3, last, 0)

    gain_copy.wait()
    places = lax.broadcasted_iota(jnp.int32, (8, LANES), 1)
    squares = jnp.zeros((8, LANES), jnp.float32)
    for c in range(cuts):
        arrived(came.at[n - 2, c], sr.at[n - 2, c])
        at = slice(c * pair, (c + 1) * pair)
        mixed = mix_ref[0, at, :] + came[n - 2, c].reshape(pair, width).astype(jnp.float32)
        mix_ref[0, at, :] = mixed
        folded = sum(
            mixed[:, k : k + LANES] * mixed[:, k : k + LANES] for k in range(0, width, LANES)
        )
        for g in range(pair // 8):
            line = jnp.sum(folded[g * 8 : (g + 1) * 8, :], axis=1, keepdims=True)
            squares = jnp.where(places == c * (pair // 8) + g, line, squares)
    sq_ref[...] = squares
    for k in range(1, tps):
        remote(
            sq_ref, sq_got.at[k - 1], ends.at[4], qr.at[0], (me, lax.rem(mine + k, tps))
        ).start()
    arrived(xall.at[pl.ds(1, n - 1)], ends.at[0])
    arrived(metas.at[pl.ds(1, n - 1)], ends.at[1])
    arrived(got_ref, ends.at[2])
    arrived(sent, ends.at[3])
    arrived(sq_got, qr.at[0])
    total = squares
    for k in range(1, tps):
        total = total + sq_got[k - 1]
    scale = lax.rsqrt(total / (width * tps) + 1e-06)
    gain = gain_ref[...]
    for g in range(0, block // 8, 2):
        column = jnp.concatenate([scale[:, g : g + 1], scale[:, g + 1 : g + 2]], axis=0)
        c, within = divmod(g * 8, pair)
        d, r = divmod(within, rows)
        token = d * half + c * rows + r
        out_ref[token : token + 16, :] = (
            mix_ref[0, g * 8 : g * 8 + 16, :] * column * gain
        ).astype(jnp.bfloat16)
    arrived(sq_got, ends.at[4])


def body(tokens, row_ids, row_gates, key_table, value_table, norm_gain):
    block, width = tokens.shape
    picks = row_ids.shape[1]
    experts = key_table.shape[0]
    n, tps = lax.axis_size("ep"), lax.axis_size("tp")
    half = block // 2
    lines = half * picks // ROW
    cuts = 4
    rows = half // cuts
    whole = pl.BlockSpec(memory_space=pltpu.VMEM)
    hbm = pl.BlockSpec(memory_space=pl.ANY)
    dma = pltpu.SemaphoreType.DMA
    bf16, f32 = jnp.bfloat16, jnp.float32
    return pl.pallas_call(
        functools.partial(kernel, n, tps, picks, cycle_of(n)),
        out_shape=pltpu.VMEM((block, width), bf16),
        in_specs=[hbm] * 6,
        out_specs=whole,
        scratch_shapes=[
            pltpu.VMEM((experts, width), bf16),
            pltpu.VMEM((experts, width), bf16),
            pltpu.VMEM((n, cuts, 2, rows, width), bf16),
            pltpu.VMEM((n, 2, 2 * lines, ROW), f32),
            pltpu.VMEM((block, experts), f32),
            pltpu.VMEM((n, 2 * lines, ROW), f32),
            pltpu.VMEM((n, tps - 1, 2 * lines, ROW), f32),
            pltpu.VMEM((block, experts), bf16),
            pltpu.VMEM((2, block, width), f32),
            pltpu.VMEM((n - 1, cuts, 2, rows, width), bf16),
            pltpu.VMEM((n - 1, cuts, 2, rows, width), bf16),
            pltpu.VMEM((8, LANES), f32),
            pltpu.VMEM((tps - 1, 8, LANES), f32),
            pltpu.VMEM((picks, block), jnp.int32),
            pltpu.VMEM((picks, block), f32),
            pltpu.VMEM((1, width), f32),
            dma((n - 1, cuts)),
            dma((n - 1,)),
            dma((n,)),
            dma((n - 1, cuts)),
            dma((1,)),
            dma((5,)),
            dma((6,)),
        ],
        compiler_params=pltpu.CompilerParams(collective_id=0, has_side_effects=True),
    )(tokens, row_ids.T, row_gates.T, key_table, value_table, norm_gain.reshape(1, -1))


def solution(mesh):
    in_specs = (P("ep", "tp"), P("ep", None), P("ep", None), P("ep", "tp"), P("ep", "tp"), P("tp"))
    out_specs = P("ep", "tp")
    return jax.shard_map(body, mesh=mesh, in_specs=in_specs, out_specs=out_specs, check_vma=False)
```

```python
import functools

import jax
import jax.numpy as jnp
from jax import lax
from jax.experimental import pallas as pl
from jax.experimental.pallas import tpu as pltpu
from jax.sharding import PartitionSpec as P

ROW = 256
LANES = 128
MESH = pl.DeviceIdType.MESH


def cycle_of(n):
    x = 1
    while 4 * x * x <= n:
        x *= 2
    z = n // x
    if x == 1 or z % 2:
        return list(range(n))
    out = []
    for row in range(z):
        cols = range(1, x) if row % 2 == 0 else range(x - 1, 0, -1)
        out += [row * x + col for col in cols]
    return out + [row * x for row in range(z - 1, -1, -1)]


def look(table, i):
    n = len(table)
    total = 0
    for k, v in enumerate(table):
        total = total + v * ((n * n - (i - k) * (i - k)) // (n * n))
    return total


def hello(n, tps, me, order):
    pos = look([order.index(i) for i in range(n)], me)
    right = look(order, lax.rem(pos + 1, n))
    left = look(order, lax.rem(pos + n - 1, n))
    mine = lax.axis_index("tp")
    barrier = pltpu.get_barrier_semaphore()
    for peer in (left, right):
        pl.semaphore_signal(barrier, inc=1, device_id=(peer, mine), device_id_type=MESH)
    for k in range(1, tps):
        pl.semaphore_signal(
            barrier, inc=1, device_id=(me, lax.rem(mine + k, tps)), device_id_type=MESH
        )
    return right, left, mine


def greeted(tps):
    pl.semaphore_wait(pltpu.get_barrier_semaphore(), 2 + tps - 1)


def remote(src, dst, send, recv, device):
    return pltpu.make_async_remote_copy(
        src_ref=src, dst_ref=dst, send_sem=send, recv_sem=recv, device_id=device, device_id_type=MESH
    )


def kernel(n, tps, picks, order, *refs):
    x_hbm, ids_hbm, gates_hbm, key_hbm, value_hbm, gain_hbm, out_ref = refs[:7]
    key_ref, value_ref, xall, metas, s_ref, part, got_ref, w_ref = refs[7:15]
    mix_ref, sent, came, sq_ref, sq_got = refs[15:20]
    ids_ref, gates_ref, gain_ref = refs[20:23]
    xr, mr, pr, sr, qr, ends, kv = refs[23:]
    cuts, rows, width = xall.shape[1], xall.shape[3], xall.shape[4]
    pair = 2 * rows
    block = cuts * pair
    half = block // 2
    experts = key_ref.shape[0]
    lines = metas.shape[2] // 2
    me = lax.axis_index("ep")
    right, left, mine = hello(n, tps, me, order)
    ids_copy = pltpu.make_async_copy(ids_hbm, ids_ref, kv.at[0])
    gates_copy = pltpu.make_async_copy(gates_hbm, gates_ref, kv.at[1])
    key_copy = pltpu.make_async_copy(key_hbm, key_ref, kv.at[3])
    value_copy = pltpu.make_async_copy(value_hbm, value_ref, kv.at[4])
    gain_copy = pltpu.make_async_copy(gain_hbm, gain_ref, kv.at[5])
    ids_copy.start()
    gates_copy.start()
    for c in range(cuts):
        for d in (0, 1):
            pltpu.make_async_copy(
                x_hbm.at[pl.ds(d * half + c * rows, rows)], xall.at[0, c, d], kv.at[2]
            ).start()
    for copy in (key_copy, value_copy, gain_copy):
        copy.start()
    base = me * experts
    peers = (right, left)
    near = n - 2

    def x_copy(d, step, c):
        return remote(
            xall.at[step, c, d],
            xall.at[step + 1, c, d],
            ends.at[0],
            xr.at[step, c],
            (peers[d], mine),
        )

    def m_copy(d, step):
        return remote(
            metas.at[step, d], metas.at[step + 1, d], ends.at[1], mr.at[step], (peers[d], mine)
        )

    def far_copy(d, c):
        return remote(
            xall.at[0, c, 1 - d], xall.at[n - 1, c, 1 - d], ends.at[0], xr.at[near, c], (peers[d], mine)
        )

    def far_meta(d):
        return remote(
            metas.at[0, 1 - d], metas.at[n - 1, 1 - d], ends.at[1], mr.at[near], (peers[d], mine)
        )

    def p_copy(s, k):
        return remote(
            part.at[s],
            got_ref.at[s, k - 1],
            ends.at[2],
            pr.at[s],
            (me, lax.rem(mine + k, tps)),
        )

    def r_copy(d, s, c):
        return remote(
            sent.at[s, c, d], came.at[s, c, d], ends.at[3], sr.at[s, c], (peers[d], mine)
        )

    def arrived(ref, sem):
        pltpu.make_async_copy(ref, ref, sem).wait()

    per_half = LANES // picks
    per = ROW // picks
    pick_row = lax.broadcasted_iota(jnp.int32, (picks, LANES), 0)
    pick_lane = lax.broadcasted_iota(jnp.int32, (picks, LANES), 1) // per_half
    ids_copy.wait()
    gates_copy.wait()
    for which, table in enumerate((ids_ref[...].astype(jnp.float32), gates_ref[...])):
        for tile in range(block // LANES):
            slanted = pltpu.roll(
                table[:, tile * LANES : (tile + 1) * LANES], 0, 1, stride=per_half, stride_axis=0
            )
            for g in range(picks):
                moved = pltpu.roll(slanted, (LANES - g * per_half) % LANES, 1) if g else slanted
                line = jnp.sum(
                    jnp.where(pick_row == pick_lane, moved, 0.0), axis=0, keepdims=True
                )
                i, h2 = divmod(tile * picks + g, 2)
                d, r = divmod(i, lines)
                metas[
                    0, d, which * lines + r : which * lines + r + 1, h2 * LANES : (h2 + 1) * LANES
                ] = line
    arrived(xall.at[0], kv.at[2])
    greeted(tps)
    for c in range(cuts):
        for d in (0, 1):
            x_copy(d, 0, c).start()
            if c == 0:
                m_copy(d, 0).start()

    sub = lax.broadcasted_iota(jnp.int32, (per_half, LANES), 0)
    lane = lax.broadcasted_iota(jnp.int32, (per_half, LANES), 1)
    own_lane = sub == lane % per_half
    tall = experts // ROW * per
    flat = lax.broadcasted_iota(jnp.int32, (1, ROW), 1)
    lane_token = flat // LANES * per_half + flat % per_half
    tall_iota = lax.broadcasted_iota(jnp.int32, (tall, ROW), 0)
    lo_iota = lax.broadcasted_iota(jnp.int32, (ROW, ROW), 0)
    spans = 2 * lines
    wide = experts // spans
    each = rows // per

    def place(i):
        return i // each % 2, i // (2 * each) * each + i % each

    def gather_on(s, c):
        @pl.when(s <= near)
        def _():
            arrived(xall.at[s, c], xr.at[s - 1, c])

            @pl.when(s < near)
            def _():
                for d in (0, 1):
                    x_copy(d, s, c).start()

            if c == 0:
                arrived(metas.at[s], mr.at[s - 1])

                @pl.when(s < near)
                def _():
                    for d in (0, 1):
                        m_copy(d, s).start()

    def far_start(c):
        for d in (0, 1):
            far_copy(d, c).start()
            if c == 0:
                far_meta(d).start()

    def far_end():
        arrived(metas.at[n - 1], mr.at[near])
        for c in range(cuts):
            arrived(xall.at[n - 1, c], xr.at[near, c])

    def score(s, i):
        at = slice(i * wide, (i + 1) * wide)
        s_ref[:, at] = lax.dot_general(
            xall[s].reshape(block, width),
            key_ref[at, :],
            (((1,), (1,)), ((), ())),
            preferred_element_type=jnp.float32,
        )

    def choose(s, i):
        d, r = place(i)
        for h2 in range(ROW // LANES):
            lanes = slice(h2 * LANES, (h2 + 1) * LANES)
            ids = metas[s, d, r : r + 1, lanes].astype(jnp.int32) - base
            ids = jnp.broadcast_to(ids, (per_half, LANES))
            owned = (ids >= 0) & (ids < experts)
            hi = jnp.where(owned, ids >> 7, -1)
            lo = jnp.where(owned, ids & (LANES - 1), 0)
            row = i * per + h2 * per_half
            acc = jnp.zeros((per_half, LANES), jnp.float32)
            for h in range(experts // LANES):
                tile = s_ref[row : row + per_half, h * LANES : (h + 1) * LANES]
                acc = jnp.where(hi == h, jnp.take_along_axis(tile, lo, axis=1), acc)
            part[s, i : i + 1, lanes] = jnp.sum(
                jnp.where(own_lane, acc, 0.0), axis=0, keepdims=True
            )

    def build(s, i):
        d, r = place(i)
        total = part[s, i : i + 1, :]
        for k in range(1, tps):
            total = total + got_ref[s, k - 1, i : i + 1, :]
        gate = metas[s, d, lines + r : lines + r + 1, :]
        h = 0.5 * total * (1.0 + lax.erf(total * (0.5**0.5))) * gate
        ids = metas[s, d, r : r + 1, :].astype(jnp.int32) - base
        owned = (ids >= 0) & (ids < experts)
        code = jnp.where(owned, (ids >> 8) * per + lane_token, -1)
        lo = ids & (ROW - 1)
        a = jnp.where(tall_iota == code, h, 0.0).astype(jnp.bfloat16)
        b = jnp.where(lo_iota == lo, 1.0, 0.0).astype(jnp.bfloat16)
        w = lax.dot_general(
            a, b, (((1,), (1,)), ((), ())), preferred_element_type=jnp.float32
        ).astype(jnp.bfloat16)
        for c in range(experts // ROW):
            w_ref[i * per : (i + 1) * per, c * ROW : (c + 1) * ROW] = w[c * per : (c + 1) * per, :]

    def send_part(s):
        for k in range(1, tps):
            p_copy(s, k).start()

    def wait_part(s):
        arrived(got_ref.at[s], pr.at[s])

    def blend(s, q, choosing):
        pieces = 2
        deep = experts // (2 * pieces)
        mixed = None
        for p in range(pieces):
            at = slice((q * pieces + p) * deep, (q * pieces + p + 1) * deep)
            dot = jnp.dot(w_ref[:, at], value_ref[at, :], preferred_element_type=jnp.float32)
            mixed = dot if mixed is None else mixed + dot
            if choosing is not None:
                count = spans // (2 * pieces)
                for i in range((q * pieces + p) * count, (q * pieces + p + 1) * count):
                    choose(choosing, i)
        slot = lax.rem(s, 2)
        mix_ref[slot] = mixed if q == 0 else mix_ref[slot] + mixed

    def reduce_on(s, c):
        @pl.when(s == 1)
        def _():
            at = slice(c * pair, (c + 1) * pair)
            sent[0, c] = mix_ref[1, at, :].astype(jnp.bfloat16).reshape(2, rows, width)
            for d in (0, 1):
                r_copy(d, 0, c).start()

        @pl.when(s >= 2)
        def _():
            pass_sum(s, c)

    def pass_sum(s, c):
        at = slice(c * pair, (c + 1) * pair)
        arrived(came.at[s - 2, c], sr.at[s - 2, c])
        before = came[s - 2, c].reshape(pair, width).astype(jnp.float32)
        share = mix_ref[lax.rem(s, 2), at, :]
        sent[s - 1, c] = (share + before).astype(jnp.bfloat16).reshape(2, rows, width)
        for d in (0, 1):
            r_copy(d, s - 1, c).start()

    key_copy.wait()
    far_start(0)
    for i in range(spans):
        score(0, i)
    for i in range(spans):
        choose(0, i)
    send_part(0)
    for c in range(cuts):
        gather_on(1, c)

    def lead(t, carry):
        for q in range(cuts):
            part_of = spans * 2 // cuts
            for i in range(q * part_of, (q + 1) * part_of):
                if i < spans:
                    score(t, i)
                else:
                    choose(t, i - spans)
            if q == cuts - 1:
                send_part(t)
            gather_on(t + 1, q)
        return carry

    lax.fori_loop(1, 3, lead, 0)
    value_copy.wait()

    def steady(t, carry):
        wait_part(t - 2)
        for q in (0, 1):
            for i in range(q * spans // 2, (q + 1) * spans // 2):
                score(t, i)
                build(t - 2, i)
            gather_on(t + 1, q)
            if q == 1:

                @pl.when(t == 3)
                def _():
                    far_start(1)

            reduce_on(t - 3, 1 + q)
        blend(t - 2, 0, t)
        gather_on(t + 1, 2)

        @pl.when(t == near - 1)
        def _():
            far_start(2)

        reduce_on(t - 3, 3)
        blend(t - 2, 1, t)
        send_part(t)
        gather_on(t + 1, 3)
        reduce_on(t - 2, 0)

        @pl.when(t == near - 1)
        def _():
            far_start(3)

        return carry

    lax.fori_loop(3, near, steady, 0)

    def late(t, carry):
        wait_part(t - 2)
        for q in (0, 1):
            for i in range(q * spans // 2, (q + 1) * spans // 2):
                score(t, i)
                build(t - 2, i)
            pass_sum(t - 3, 1 + q)
        blend(t - 2, 0, t)
        pass_sum(t - 3, 3)
        blend(t - 2, 1, t)
        send_part(t)
        pass_sum(t - 2, 0)

        @pl.when(t == near)
        def _():
            far_end()

        return carry

    lax.fori_loop(near, n, late, 0)

    def last(t, carry):
        wait_part(t - 2)
        for q in (0, 1):
            for i in range(q * spans // 2, (q + 1) * spans // 2):
                build(t - 2, i)
            pass_sum(t - 3, 1 + q)
        blend(t - 2, 0, None)
        pass_sum(t - 3, 3)
        blend(t - 2, 1, None)
        pass_sum(t - 2, 0)
        return carry

    lax.fori_loop(n, n + 2, last, 0)
    wait_part(0)
    for q in (0, 1):
        for i in range(q * spans // 2, (q + 1) * spans // 2):
            build(0, i)
        pass_sum(n - 1, 1 + q)
    blend(0, 0, None)
    pass_sum(n - 1, 3)
    blend(0, 1, None)

    gain_copy.wait()
    places = lax.broadcasted_iota(jnp.int32, (8, LANES), 1)
    squares = jnp.zeros((8, LANES), jnp.float32)
    for c in range(cuts):
        arrived(came.at[n - 2, c], sr.at[n - 2, c])
        at = slice(c * pair, (c + 1) * pair)
        mixed = mix_ref[0, at, :] + came[n - 2, c].reshape(pair, width).astype(jnp.float32)
        mix_ref[0, at, :] = mixed
        folded = sum(
            mixed[:, k : k + LANES] * mixed[:, k : k + LANES] for k in range(0, width, LANES)
        )
        for g in range(pair // 8):
            line = jnp.sum(folded[g * 8 : (g + 1) * 8, :], axis=1, keepdims=True)
            squares = jnp.where(places == c * (pair // 8) + g, line, squares)
    sq_ref[...] = squares
    for k in range(1, tps):
        remote(
            sq_ref, sq_got.at[k - 1], ends.at[4], qr.at[0], (me, lax.rem(mine + k, tps))
        ).start()
    arrived(xall.at[pl.ds(1, n - 1)], ends.at[0])
    arrived(metas.at[pl.ds(1, n - 1)], ends.at[1])
    arrived(got_ref, ends.at[2])
    arrived(sent, ends.at[3])
    arrived(sq_got, qr.at[0])
    total = squares
    for k in range(1, tps):
        total = total + sq_got[k - 1]
    scale = lax.rsqrt(total / (width * tps) + 1e-06)
    gain = gain_ref[...]
    for g in range(0, block // 8, 2):
        column = jnp.concatenate([scale[:, g : g + 1], scale[:, g + 1 : g + 2]], axis=0)
        c, within = divmod(g * 8, pair)
        d, r = divmod(within, rows)
        token = d * half + c * rows + r
        out_ref[token : token + 16, :] = (
            mix_ref[0, g * 8 : g * 8 + 16, :] * column * gain
        ).astype(jnp.bfloat16)
    arrived(sq_got, ends.at[4])


def body(tokens, row_ids, row_gates, key_table, value_table, norm_gain):
    block, width = tokens.shape
    picks = row_ids.shape[1]
    experts = key_table.shape[0]
    n, tps = lax.axis_size("ep"), lax.axis_size("tp")
    half = block // 2
    lines = half * picks // ROW
    cuts = 4
    rows = half // cuts
    whole = pl.BlockSpec(memory_space=pltpu.VMEM)
    hbm = pl.BlockSpec(memory_space=pl.ANY)
    dma = pltpu.SemaphoreType.DMA
    bf16, f32 = jnp.bfloat16, jnp.float32
    return pl.pallas_call(
        functools.partial(kernel, n, tps, picks, cycle_of(n)),
        out_shape=pltpu.VMEM((block, width), bf16),
        in_specs=[hbm] * 6,
        out_specs=whole,
        scratch_shapes=[
            pltpu.VMEM((experts, width), bf16),
            pltpu.VMEM((experts, width), bf16),
            pltpu.VMEM((n, cuts, 2, rows, width), bf16),
            pltpu.VMEM((n, 2, 2 * lines, ROW), f32),
            pltpu.VMEM((block, experts), f32),
            pltpu.VMEM((n, 2 * lines, ROW), f32),
            pltpu.VMEM((n, tps - 1, 2 * lines, ROW), f32),
            pltpu.VMEM((block, experts), bf16),
            pltpu.VMEM((2, block, width), f32),
            pltpu.VMEM((n - 1, cuts, 2, rows, width), bf16),
            pltpu.VMEM((n - 1, cuts, 2, rows, width), bf16),
            pltpu.VMEM((8, LANES), f32),
            pltpu.VMEM((tps - 1, 8, LANES), f32),
            pltpu.VMEM((picks, block), jnp.int32),
            pltpu.VMEM((picks, block), f32),
            pltpu.VMEM((1, width), f32),
            dma((n - 1, cuts)),
            dma((n - 1,)),
            dma((n,)),
            dma((n - 1, cuts)),
            dma((1,)),
            dma((5,)),
            dma((6,)),
        ],
        compiler_params=pltpu.CompilerParams(collective_id=0, has_side_effects=True),
    )(tokens, row_ids.T, row_gates.T, key_table, value_table, norm_gain.reshape(1, -1))


def solution(mesh):
    in_specs = (P("ep", "tp"), P("ep", None), P("ep", None), P("ep", "tp"), P("ep", "tp"), P("tp"))
    out_specs = P("ep", "tp")
    return jax.shard_map(body, mesh=mesh, in_specs=in_specs, out_specs=out_specs, check_vma=False)
```

```python
import functools

import jax
import jax.numpy as jnp
from jax import lax
from jax.experimental import pallas as pl
from jax.experimental.pallas import tpu as pltpu
from jax.sharding import PartitionSpec as P

ROW = 256
LANES = 128
MESH = pl.DeviceIdType.MESH


def cycle_of(n):
    x = 1
    while 4 * x * x <= n:
        x *= 2
    z = n // x
    if x == 1 or z % 2:
        return list(range(n))
    out = []
    for row in range(z):
        cols = range(1, x) if row % 2 == 0 else range(x - 1, 0, -1)
        out += [row * x + col for col in cols]
    return out + [row * x for row in range(z - 1, -1, -1)]


def look(table, i):
    n = len(table)
    total = 0
    for k, v in enumerate(table):
        total = total + v * ((n * n - (i - k) * (i - k)) // (n * n))
    return total


def hello(n, tps, me, order):
    pos = look([order.index(i) for i in range(n)], me)
    right = look(order, lax.rem(pos + 1, n))
    left = look(order, lax.rem(pos + n - 1, n))
    mine = lax.axis_index("tp")
    barrier = pltpu.get_barrier_semaphore()
    for peer in (left, right):
        pl.semaphore_signal(barrier, inc=1, device_id=(peer, mine), device_id_type=MESH)
    for k in range(1, tps):
        pl.semaphore_signal(
            barrier, inc=1, device_id=(me, lax.rem(mine + k, tps)), device_id_type=MESH
        )
    return right, left, mine


def greeted(tps):
    pl.semaphore_wait(pltpu.get_barrier_semaphore(), 2 + tps - 1)


def remote(src, dst, send, recv, device):
    return pltpu.make_async_remote_copy(
        src_ref=src, dst_ref=dst, send_sem=send, recv_sem=recv, device_id=device, device_id_type=MESH
    )


def kernel(n, tps, picks, order, *refs):
    x_hbm, ids_hbm, gates_hbm, key_hbm, value_hbm, gain_hbm, out_ref = refs[:7]
    key_ref, value_ref, xall, metas, s_ref, part, got_ref, w_ref = refs[7:15]
    mix_ref, sent, came, sq_ref, sq_got = refs[15:20]
    ids_ref, gates_ref, gain_ref = refs[20:23]
    xr, mr, tr, pr, sr, qr, ends, kv = refs[23:]
    cuts, rows, width = xall.shape[1], xall.shape[3], xall.shape[4]
    pair = 2 * rows
    block = cuts * pair
    half = block // 2
    experts = key_ref.shape[0]
    group = metas.shape[3]
    lines = group * metas.shape[1] // 2
    me = lax.axis_index("ep")
    right, left, mine = hello(n, tps, me, order)
    ids_copy = pltpu.make_async_copy(ids_hbm, ids_ref, kv.at[0])
    gates_copy = pltpu.make_async_copy(gates_hbm, gates_ref, kv.at[1])
    key_copy = pltpu.make_async_copy(key_hbm, key_ref, kv.at[3])
    value_copy = pltpu.make_async_copy(value_hbm, value_ref, kv.at[4])
    gain_copy = pltpu.make_async_copy(gain_hbm, gain_ref, kv.at[5])
    ids_copy.start()
    gates_copy.start()
    for c in range(cuts):
        for d in (0, 1):
            pltpu.make_async_copy(
                x_hbm.at[pl.ds(d * half + c * rows, rows)], xall.at[0, c, d], kv.at[2]
            ).start()
    for copy in (key_copy, value_copy, gain_copy):
        copy.start()
    base = me * experts
    peers = (right, left)
    near = n - 2

    def x_copy(d, step, c):
        return remote(
            xall.at[step, c, d],
            xall.at[step + 1, c, d],
            ends.at[0],
            xr.at[lax.rem(step, 2), c],
            (peers[d], mine),
        )

    def m_copy(d, step):
        return remote(
            metas.at[step, mine, d],
            metas.at[step + 1, mine, d],
            ends.at[1],
            mr.at[lax.rem(step, 2)],
            (peers[d], mine),
        )

    def share_meta(s):
        for k in range(1, tps):
            remote(
                metas.at[s, mine],
                metas.at[s, mine],
                ends.at[5],
                tr.at[s - 1],
                (me, lax.rem(mine + k, tps)),
            ).start()

    def wait_meta(s):
        arrived(metas.at[s, pl.ds(0, tps - 1)], tr.at[s - 1])

    def far_copy(d, c):
        return remote(
            xall.at[0, c, 1 - d], xall.at[n - 1, c, 1 - d], ends.at[0], xr.at[2, c], (peers[d], mine)
        )

    def far_meta(d):
        return remote(
            metas.at[0, mine, 1 - d],
            metas.at[n - 1, mine, 1 - d],
            ends.at[1],
            mr.at[2],
            (peers[d], mine),
        )

    def p_copy(s, k):
        return remote(
            part.at[s],
            got_ref.at[s, k - 1],
            ends.at[2],
            pr.at[s],
            (me, lax.rem(mine + k, tps)),
        )

    def r_copy(d, s, c):
        return remote(
            sent.at[s, c, d], came.at[s, c, d], ends.at[3], sr.at[lax.rem(s, 2), c], (peers[d], mine)
        )

    def arrived(ref, sem):
        pltpu.make_async_copy(ref, ref, sem).wait()

    per_half = LANES // picks
    per = ROW // picks
    pick_row = lax.broadcasted_iota(jnp.int32, (picks, LANES), 0)
    pick_lane = lax.broadcasted_iota(jnp.int32, (picks, LANES), 1) // per_half
    arrived(xall.at[0], kv.at[2])
    greeted(tps)
    for c in range(cuts // 2):
        for d in (0, 1):
            x_copy(d, 0, c).start()
    ids_copy.wait()
    gates_copy.wait()
    for which, table in enumerate((ids_ref[...].astype(jnp.float32), gates_ref[...])):
        for tile in range(block // LANES):
            slanted = pltpu.roll(
                table[:, tile * LANES : (tile + 1) * LANES], 0, 1, stride=per_half, stride_axis=0
            )
            for g in range(picks):
                moved = pltpu.roll(slanted, (LANES - g * per_half) % LANES, 1) if g else slanted
                line = jnp.sum(
                    jnp.where(pick_row == pick_lane, moved, 0.0), axis=0, keepdims=True
                )
                i, h2 = divmod(tile * picks + g, 2)
                d, r = divmod(i, lines)
                q, r = divmod(which * lines + r, group)
                metas[0, q, d, r : r + 1, h2 * LANES : (h2 + 1) * LANES] = line
    for d in (0, 1):
        m_copy(d, 0).start()
    for c in range(cuts // 2, cuts):
        for d in (0, 1):
            x_copy(d, 0, c).start()

    sub = lax.broadcasted_iota(jnp.int32, (per_half, LANES), 0)
    lane = lax.broadcasted_iota(jnp.int32, (per_half, LANES), 1)
    own_lane = sub == lane % per_half
    tall = experts // ROW * per
    flat = lax.broadcasted_iota(jnp.int32, (1, ROW), 1)
    lane_token = flat // LANES * per_half + flat % per_half
    tall_iota = lax.broadcasted_iota(jnp.int32, (tall, ROW), 0)
    lo_iota = lax.broadcasted_iota(jnp.int32, (ROW, ROW), 0)
    spans = 2 * lines
    wide = experts // spans
    each = rows // per

    def place(i):
        return i // each % 2, i // (2 * each) * each + i % each

    def meta_row(s, d, r):
        return metas[s, r // group, d, r % group : r % group + 1, :]

    def gather_on(s, c):
        @pl.when(s <= near)
        def _():
            arrived(xall.at[s, c], xr.at[lax.rem(s - 1, 2), c])

            @pl.when(s < near)
            def _():
                for d in (0, 1):
                    x_copy(d, s, c).start()

            if c == 0:
                arrived(metas.at[s, mine], mr.at[lax.rem(s - 1, 2)])

                @pl.when(s < near)
                def _():
                    for d in (0, 1):
                        m_copy(d, s).start()

                share_meta(s)

    def far_start(c):
        for d in (0, 1):
            far_copy(d, c).start()

    def far_end():
        for c in range(cuts):
            arrived(xall.at[n - 1, c], xr.at[2, c])

    def score(s, i):
        at = slice(i * wide, (i + 1) * wide)
        s_ref[:, at] = lax.dot_general(
            xall[s].reshape(block, width),
            key_ref[at, :],
            (((1,), (1,)), ((), ())),
            preferred_element_type=jnp.float32,
        )

    def choose(s, i):
        d, r = place(i)
        for h2 in range(ROW // LANES):
            lanes = slice(h2 * LANES, (h2 + 1) * LANES)
            ids = meta_row(s, d, r)[:, lanes].astype(jnp.int32) - base
            ids = jnp.broadcast_to(ids, (per_half, LANES))
            owned = (ids >= 0) & (ids < experts)
            hi = jnp.where(owned, ids >> 7, -1)
            lo = jnp.where(owned, ids & (LANES - 1), 0)
            row = i * per + h2 * per_half
            acc = jnp.zeros((per_half, LANES), jnp.float32)
            for h in range(experts // LANES):
                tile = s_ref[row : row + per_half, h * LANES : (h + 1) * LANES]
                acc = jnp.where(hi == h, jnp.take_along_axis(tile, lo, axis=1), acc)
            part[s, i : i + 1, lanes] = jnp.sum(
                jnp.where(own_lane, acc, 0.0), axis=0, keepdims=True
            )

    def build(s, i):
        d, r = place(i)
        total = part[s, i : i + 1, :]
        for k in range(1, tps):
            total = total + got_ref[s, k - 1, i : i + 1, :]
        gate = meta_row(s, d, lines + r)
        h = 0.5 * total * (1.0 + lax.erf(total * (0.5**0.5))) * gate
        ids = meta_row(s, d, r).astype(jnp.int32) - base
        owned = (ids >= 0) & (ids < experts)
        code = jnp.where(owned, (ids >> 8) * per + lane_token, -1)
        lo = ids & (ROW - 1)
        a = jnp.where(tall_iota == code, h, 0.0).astype(jnp.bfloat16)
        b = jnp.where(lo_iota == lo, 1.0, 0.0).astype(jnp.bfloat16)
        w = lax.dot_general(
            a, b, (((1,), (1,)), ((), ())), preferred_element_type=jnp.float32
        ).astype(jnp.bfloat16)
        for c in range(experts // ROW):
            w_ref[i * per : (i + 1) * per, c * ROW : (c + 1) * ROW] = w[c * per : (c + 1) * per, :]

    def send_part(s):
        for k in range(1, tps):
            p_copy(s, k).start()

    def wait_part(s):
        arrived(got_ref.at[s], pr.at[s])

    def blend(s, q, choosing):
        pieces = 2
        deep = experts // (2 * pieces)
        mixed = None
        for p in range(pieces):
            at = slice((q * pieces + p) * deep, (q * pieces + p + 1) * deep)
            dot = jnp.dot(w_ref[:, at], value_ref[at, :], preferred_element_type=jnp.float32)
            mixed = dot if mixed is None else mixed + dot
            if choosing is not None:
                count = spans // (2 * pieces)
                for i in range((q * pieces + p) * count, (q * pieces + p + 1) * count):
                    choose(choosing, i)
        slot = lax.rem(s, 2)
        mix_ref[slot] = mixed if q == 0 else mix_ref[slot] + mixed

    def reduce_on(s, c):
        @pl.when(s == 1)
        def _():
            at = slice(c * pair, (c + 1) * pair)
            sent[0, c] = mix_ref[1, at, :].astype(jnp.bfloat16).reshape(2, rows, width)
            for d in (0, 1):
                r_copy(d, 0, c).start()

        @pl.when(s >= 2)
        def _():
            pass_sum(s, c)

    def pass_sum(s, c):
        at = slice(c * pair, (c + 1) * pair)
        arrived(came.at[s - 2, c], sr.at[lax.rem(s - 2, 2), c])
        before = came[s - 2, c].reshape(pair, width).astype(jnp.float32)
        share = mix_ref[lax.rem(s, 2), at, :]
        sent[s - 1, c] = (share + before).astype(jnp.bfloat16).reshape(2, rows, width)
        for d in (0, 1):
            r_copy(d, s - 1, c).start()

    key_copy.wait()
    for i in range(spans):
        score(0, i)
    for i in range(spans):
        choose(0, i)
    send_part(0)
    for c in range(cuts):
        gather_on(1, c)

    def lead(t, carry):
        for q in range(cuts):
            part_of = spans * 2 // cuts
            for i in range(q * part_of, (q + 1) * part_of):
                if i == spans:
                    wait_meta(t)
                if i < spans:
                    score(t, i)
                else:
                    choose(t, i - spans)
            if q == cuts - 1:
                send_part(t)
            gather_on(t + 1, q)
        return carry

    lax.fori_loop(1, 3, lead, 0)
    value_copy.wait()

    def steady(t, carry):
        wait_part(t - 2)
        for q in (0, 1):
            for i in range(q * spans // 2, (q + 1) * spans // 2):
                score(t, i)
                build(t - 2, i)
            gather_on(t + 1, q)
            reduce_on(t - 3, 1 + q)
            if q == 0:

                @pl.when(t == 3)
                def _():
                    for d in (0, 1):
                        far_meta(d).start()

                @pl.when(t == near - 1)
                def _():
                    arrived(metas.at[n - 1, mine], mr.at[2])
                    share_meta(n - 1)
                    far_start(2)

            else:

                @pl.when(t == 3)
                def _():
                    far_start(0)
                    far_start(1)

                @pl.when(t == near - 1)
                def _():
                    far_start(3)

        wait_meta(t)
        blend(t - 2, 0, t)
        gather_on(t + 1, 2)
        reduce_on(t - 3, 3)

        blend(t - 2, 1, t)
        send_part(t)
        gather_on(t + 1, 3)
        reduce_on(t - 2, 0)
        return carry

    lax.fori_loop(3, near, steady, 0)

    def late(t, carry):
        wait_part(t - 2)
        for q in (0, 1):
            for i in range(q * spans // 2, (q + 1) * spans // 2):
                score(t, i)
                build(t - 2, i)
            pass_sum(t - 3, 1 + q)
        wait_meta(t)
        blend(t - 2, 0, t)
        pass_sum(t - 3, 3)
        blend(t - 2, 1, t)
        send_part(t)
        pass_sum(t - 2, 0)

        @pl.when(t == near)
        def _():
            far_end()

        return carry

    lax.fori_loop(near, n, late, 0)

    def last(t, carry):
        wait_part(t - 2)
        for q in (0, 1):
            for i in range(q * spans // 2, (q + 1) * spans // 2):
                build(t - 2, i)
            pass_sum(t - 3, 1 + q)
        blend(t - 2, 0, None)
        pass_sum(t - 3, 3)
        blend(t - 2, 1, None)
        pass_sum(t - 2, 0)
        return carry

    lax.fori_loop(n, n + 2, last, 0)
    wait_part(0)
    for q in (0, 1):
        for i in range(q * spans // 2, (q + 1) * spans // 2):
            build(0, i)
        pass_sum(n - 1, 1 + q)
    blend(0, 0, None)
    pass_sum(n - 1, 3)
    blend(0, 1, None)

    gain_copy.wait()
    places = lax.broadcasted_iota(jnp.int32, (8, LANES), 1)
    squares = jnp.zeros((8, LANES), jnp.float32)
    for c in range(cuts):
        arrived(came.at[n - 2, c], sr.at[(n - 2) % 2, c])
        at = slice(c * pair, (c + 1) * pair)
        mixed = mix_ref[0, at, :] + came[n - 2, c].reshape(pair, width).astype(jnp.float32)
        mix_ref[0, at, :] = mixed
        folded = sum(
            mixed[:, k : k + LANES] * mixed[:, k : k + LANES] for k in range(0, width, LANES)
        )
        for g in range(pair // 8):
            line = jnp.sum(folded[g * 8 : (g + 1) * 8, :], axis=1, keepdims=True)
            squares = jnp.where(places == c * (pair // 8) + g, line, squares)
    sq_ref[...] = squares
    for k in range(1, tps):
        remote(
            sq_ref, sq_got.at[k - 1], ends.at[4], qr.at[0], (me, lax.rem(mine + k, tps))
        ).start()
    arrived(xall.at[pl.ds(1, n - 1)], ends.at[0])
    arrived(metas.at[pl.ds(1, n - 1), 0], ends.at[1])
    arrived(metas.at[pl.ds(1, n - 1), pl.ds(0, tps - 1)], ends.at[5])
    arrived(got_ref, ends.at[2])
    arrived(sent, ends.at[3])
    arrived(sq_got, qr.at[0])
    total = squares
    for k in range(1, tps):
        total = total + sq_got[k - 1]
    scale = lax.rsqrt(total / (width * tps) + 1e-06)
    gain = gain_ref[...]
    for g in range(0, block // 8, 2):
        column = jnp.concatenate([scale[:, g : g + 1], scale[:, g + 1 : g + 2]], axis=0)
        c, within = divmod(g * 8, pair)
        d, r = divmod(within, rows)
        token = d * half + c * rows + r
        out_ref[token : token + 16, :] = (
            mix_ref[0, g * 8 : g * 8 + 16, :] * column * gain
        ).astype(jnp.bfloat16)
    arrived(sq_got, ends.at[4])


def body(tokens, row_ids, row_gates, key_table, value_table, norm_gain):
    block, width = tokens.shape
    picks = row_ids.shape[1]
    experts = key_table.shape[0]
    n, tps = lax.axis_size("ep"), lax.axis_size("tp")
    half = block // 2
    lines = half * picks // ROW
    cuts = 4
    rows = half // cuts
    whole = pl.BlockSpec(memory_space=pltpu.VMEM)
    hbm = pl.BlockSpec(memory_space=pl.ANY)
    dma = pltpu.SemaphoreType.DMA
    bf16, f32 = jnp.bfloat16, jnp.float32
    return pl.pallas_call(
        functools.partial(kernel, n, tps, picks, cycle_of(n)),
        out_shape=pltpu.VMEM((block, width), bf16),
        in_specs=[hbm] * 6,
        out_specs=whole,
        scratch_shapes=[
            pltpu.VMEM((experts, width), bf16),
            pltpu.VMEM((experts, width), bf16),
            pltpu.VMEM((n, cuts, 2, rows, width), bf16),
            pltpu.VMEM((n, tps, 2, 2 * lines // tps, ROW), f32),
            pltpu.VMEM((block, experts), f32),
            pltpu.VMEM((n, 2 * lines, ROW), f32),
            pltpu.VMEM((n, tps - 1, 2 * lines, ROW), f32),
            pltpu.VMEM((block, experts), bf16),
            pltpu.VMEM((2, block, width), f32),
            pltpu.VMEM((n - 1, cuts, 2, rows, width), bf16),
            pltpu.VMEM((n - 1, cuts, 2, rows, width), bf16),
            pltpu.VMEM((8, LANES), f32),
            pltpu.VMEM((tps - 1, 8, LANES), f32),
            pltpu.VMEM((picks, block), jnp.int32),
            pltpu.VMEM((picks, block), f32),
            pltpu.VMEM((1, width), f32),
            dma((3, cuts)),
            dma((3,)),
            dma((n - 1,)),
            dma((n,)),
            dma((2, cuts)),
            dma((1,)),
            dma((6,)),
            dma((6,)),
        ],
        compiler_params=pltpu.CompilerParams(collective_id=0, has_side_effects=True),
    )(tokens, row_ids.T, row_gates.T, key_table, value_table, norm_gain.reshape(1, -1))


def solution(mesh):
    in_specs = (P("ep", "tp"), P("ep", None), P("ep", None), P("ep", "tp"), P("ep", "tp"), P("tp"))
    out_specs = P("ep", "tp")
    return jax.shard_map(body, mesh=mesh, in_specs=in_specs, out_specs=out_specs, check_vma=False)
```
